32 devices in a mesh: fs: 16 (over z, y, x), tp: 2 (over core).
Axes of the slice: x: 2, y: 2, z: 4, core: 2. Of those that a mesh axis runs over, the one named last changes fastest.
Arguments:
- tokens: bfloat16 [8192, 2048], P('fs', 'tp'), may hold values from -6 to 6
- norm_gain: bfloat16 [2048], P('tp'), may hold values from 0.099609375 to 1.8984375
- proj_u: bfloat16 [2048, 2048], P('fs', 'tp'), may hold values from -0.125 to 0.125
- proj_v: bfloat16 [2048, 2048], P('fs', 'tp'), may hold values from -0.125 to 0.125
- layer_gain: bfloat16 [2048], P('tp'), may hold values from 0.099609375 to 1.8984375
- layer_shift: bfloat16 [2048], P('tp'), may hold values from -3 to 3
- mix_weight: bfloat16 [16, 128, 128], P('tp'), may hold values from -0.5 to 0.5
- mix_bias: bfloat16 [16, 128], P('tp'), may hold values from 0.099609375 to 1.8984375
- proj_out: bfloat16 [2048, 2048], P('tp', 'fs'), may hold values from -0.1875 to 0.1875
- ffn_gain: bfloat16 [2048], P('tp'), may hold values from 0.099609375 to 1.8984375
- ffn_gate: bfloat16 [2048, 4096], P('fs', 'tp'), may hold values from -0.125 to 0.125
- ffn_value: bfloat16 [2048, 4096], P('fs', 'tp'), may hold values from -0.125 to 0.125
- conv_gate: bfloat16 [3, 4096], P(None, 'tp'), may hold values from -3 to 3
- conv_value: bfloat16 [3, 4096], P(None, 'tp'), may hold values from -3 to 3
- proj_down: bfloat16 [4096, 2048], P('tp', 'fs'), may hold values from -0.125 to 0.125
Outputs:
- result: bfloat16 [8192, 2048], P('fs', 'tp')
The draws below stay inside these ranges and needn't reach their ends.
All inputs are finite; a program needn't handle non-finite values.
Results may differ from the reference program's by a relative error of at most 0.017.
Values may be sent and summed in bfloat16 or wider, within the bound.
A program may use at most 64 MiB of HBM per device.

```python
import jax
import jax.numpy as jnp
from jax import lax

D = 2048
GROUPS = 16
GROUP_DIM = 128
DA = 2048
FF = 4096
BLOCK = 128
SEGMENT = 64
KERNEL = 3
SEQ_LEN = 256
TOK_DEV = 512
TOKENS = 8192
N_FS = 16
N_TP = 2


def draw_tokens(key, part):
    column = jnp.arange(D).astype(jnp.float32)
    col_scale = 0.6 * 3.0 ** (column / D)
    values = jax.random.normal(key, (TOKENS, D), jnp.float32) * col_scale
    return jnp.clip(values, -6.0, 6.0).astype(jnp.bfloat16)


def strengthened(drawn, stream_key, source, target, blocks, factor):
    owner, partner = [(jnp.arange(drawn.shape[dim]) // (drawn.shape[dim] // blocks)).reshape([-1 if axis == dim else 1 for axis in range(drawn.ndim)]) for dim in (source, target)]
    chosen = jax.random.permutation(stream_key, blocks)[partner]
    strong = (owner == chosen) | (owner == (partner + blocks // 2) % blocks)
    return jnp.where(strong, factor * drawn, drawn)


def levels(own_key, shape, shards, least, high):
    factor_of, own = 1.0, jax.random.fold_in(own_key, 6)
    for position, blocks in shards:
        draws = jnp.exp(jax.random.uniform(jax.random.fold_in(own, position), (blocks,), jnp.float32, least / len(shards), high / len(shards)))
        factor_of = factor_of * jnp.repeat(draws, shape[position] // blocks).reshape([-1 if axis == position else 1 for axis in range(len(shape))])
    return factor_of


def bell_draw(key, extent, scale, most, cuts=(), dtype=jnp.bfloat16):
    loudness = levels(key, extent, cuts, -0.22, 0.18) if cuts else 1.0
    values = jax.random.normal(key, extent, jnp.float32) * scale * loudness
    return jnp.minimum(jnp.maximum(values, -most), most).astype(dtype)


def bell_draw_with(own_key, dims, scale, most, cuts, heavy, dtype=jnp.bfloat16):
    array = scale * jax.random.normal(own_key, dims, jnp.float32)
    if cuts:
        array = array * levels(own_key, dims, cuts, -0.22, 0.18)
    return jnp.clip(strengthened(array, jax.random.fold_in(own_key, 3), *heavy), -most, most).astype(dtype)


def setup_inputs(seed: int = 0) -> dict:
    keys = jax.random.split(jax.random.key(seed), 16)
    tokens = draw_tokens(jax.random.fold_in(keys[15], 71), 0)
    norm_gain = jnp.clip(1.0 + 0.18 * jax.random.normal(keys[1], (D,), jnp.float32), 0.099609375, 1.8984375).astype(jnp.bfloat16)
    proj_u = bell_draw(keys[2], (D, DA), D ** -0.5, 0.125, ((0, 16), (1, 2)))
    proj_v = bell_draw(keys[3], (D, DA), D ** -0.5, 0.125, ((0, 16), (1, 2)))
    layer_gain = jnp.clip(1.0 + 0.18 * jax.random.normal(keys[4], (DA,), jnp.float32), 0.099609375, 1.8984375).astype(jnp.bfloat16)
    layer_shift = bell_draw(keys[5], (DA,), 0.5, 3.0, ((0, 2),))
    mix_weight = bell_draw(keys[6], (GROUPS, BLOCK, BLOCK), BLOCK ** -0.5, 0.5, ((0, 2),))
    mix_bias = jnp.clip(1.0 + 0.18 * jax.random.normal(keys[7], (GROUPS, BLOCK), jnp.float32), 0.099609375, 1.8984375).astype(jnp.bfloat16)
    proj_out = bell_draw_with(keys[8], (DA, D), DA ** -0.5, 0.1875, ((0, 2), (1, 16)), (0, 1, 16, 2.0))
    ffn_gain = jnp.clip(1.0 + 0.18 * jax.random.normal(keys[9], (D,), jnp.float32), 0.099609375, 1.8984375).astype(jnp.bfloat16)
    ffn_gate = bell_draw(keys[10], (D, FF), D ** -0.5, 0.125, ((0, 16), (1, 2)))
    ffn_value = bell_draw(keys[11], (D, FF), D ** -0.5, 0.125, ((0, 16), (1, 2)))
    conv_gate = bell_draw(keys[12], (KERNEL, FF), 0.6, 3.0, ((1, 2),))
    conv_value = bell_draw(keys[13], (KERNEL, FF), 0.6, 3.0, ((1, 2),))
    proj_down = bell_draw_with(keys[14], (FF, D), FF ** -0.5, 0.125, ((0, 2), (1, 16)), (0, 1, 16, 2.0))
    return dict(tokens=tokens, norm_gain=norm_gain, proj_u=proj_u, proj_v=proj_v, layer_gain=layer_gain, layer_shift=layer_shift, mix_weight=mix_weight, mix_bias=mix_bias, proj_out=proj_out, ffn_gain=ffn_gain, ffn_gate=ffn_gate, ffn_value=ffn_value, conv_gate=conv_gate, conv_value=conv_value, proj_down=proj_down)


EPS = 1e-06

def matmul(operand, matrix):
    return jnp.dot(operand, matrix, preferred_element_type=jnp.float32)

def share_sum(operand, matrix, share_width):
    summed = jnp.zeros((operand.shape[0], matrix.shape[1]), jnp.float32)
    for index in range(N_TP):
        lower = index * share_width
        product = matmul(operand[:, lower:lower + share_width], matrix[lower:lower + share_width, :])
        rounded = lax.optimization_barrier(product.astype(jnp.bfloat16))
        summed = summed + rounded.astype(jnp.float32)
    return summed

def rms_rows(values_in, gain_row):
    values = values_in.astype(jnp.float32)
    scale_row = lax.rsqrt(lax.optimization_barrier(jnp.mean(values * values, axis=1, keepdims=True)) + EPS)
    return (values * scale_row * gain_row.astype(jnp.float32)).astype(jnp.bfloat16)

def causal_taps(values, weights):
    seq_count = values.shape[0] // SEQ_LEN
    shaped = values.reshape(seq_count, SEQ_LEN, values.shape[1])
    padded = jnp.pad(shaped, ((0, 0), (KERNEL - 1, 0), (0, 0)))
    summed = jnp.zeros(shaped.shape, jnp.float32)
    for tap_index in range(KERNEL):
        summed = summed + padded[:, tap_index:tap_index + SEQ_LEN].astype(jnp.float32) * weights[tap_index].astype(jnp.float32)
    return summed.reshape(values.shape[0], values.shape[1])

def reference(tokens, norm_gain, proj_u, proj_v, layer_gain, layer_shift, mix_weight, mix_bias, proj_out, ffn_gain, ffn_gate, ffn_value, conv_gate, conv_value, proj_down):
    segment = jnp.arange(BLOCK) // SEGMENT
    visible = segment[None, :] <= segment[:, None]
    masked = jnp.where(visible[None], mix_weight, jnp.zeros_like(mix_weight)).astype(jnp.float32)

    def one_block(token_rows):
        row_count = token_rows.shape[0]
        normed = rms_rows(token_rows, norm_gain)
        act_u = jax.nn.gelu(matmul(normed, proj_u), approximate=False)
        act_v = jax.nn.gelu(matmul(normed, proj_v), approximate=False)
        center = lax.optimization_barrier(jnp.mean(act_v, axis=1, keepdims=True))
        spread = lax.optimization_barrier(jnp.mean(act_v * act_v, axis=1, keepdims=True)) - center * center
        mixed_in = ((act_v - center) * lax.rsqrt(spread + EPS) * layer_gain.astype(jnp.float32) + layer_shift.astype(jnp.float32)).astype(jnp.bfloat16)
        blocks = mixed_in.reshape(row_count // BLOCK, BLOCK, GROUPS, GROUP_DIM).astype(jnp.float32)
        spatial = jnp.einsum('gij,njgc->nigc', masked, blocks) + mix_bias.astype(jnp.float32).T[None, :, :, None]
        gated = (act_u * spatial.reshape(row_count, DA)).astype(jnp.bfloat16)
        stream = (token_rows.astype(jnp.float32) + share_sum(gated, proj_out, DA // N_TP)).astype(jnp.bfloat16)
        normed_two = rms_rows(stream, ffn_gain)
        up_gate = matmul(normed_two, ffn_gate).astype(jnp.bfloat16)
        up_value = matmul(normed_two, ffn_value).astype(jnp.bfloat16)
        conv_g = causal_taps(up_gate, conv_gate)
        conv_v = causal_taps(up_value, conv_value)
        hidden = (jax.nn.silu(conv_g) * conv_v).astype(jnp.bfloat16)
        return (stream.astype(jnp.float32) + share_sum(hidden, proj_down, FF // N_TP)).astype(jnp.bfloat16)
    grouped = tokens.reshape(N_FS, TOK_DEV, D)
    return lax.map(one_block, grouped).reshape(TOKENS, D)
```

```python
import jax
import jax.numpy as jnp
from jax import lax
from jax.sharding import PartitionSpec as P

GROUP_DIM = 128
BLOCK = 128
SEGMENT = 64
KERNEL = 3
SEQ_LEN = 256


EPS = 1e-06


def matmul(operand, matrix):
    return jnp.dot(operand, matrix, preferred_element_type=jnp.float32)


def local_rms(values_in, gain_row):
    values = values_in.astype(jnp.float32)
    scale_row = lax.rsqrt(jnp.mean(values * values, axis=1, keepdims=True) + EPS)
    return (values * scale_row * gain_row.astype(jnp.float32)).astype(jnp.bfloat16)


def causal_taps(values, weights):
    seq_count = values.shape[0] // SEQ_LEN
    shaped = values.reshape(seq_count, SEQ_LEN, values.shape[1])
    padded = jnp.pad(shaped, ((0, 0), (KERNEL - 1, 0), (0, 0)))
    summed = jnp.zeros(shaped.shape, jnp.float32)
    for tap_index in range(KERNEL):
        summed = summed + padded[:, tap_index : tap_index + SEQ_LEN].astype(jnp.float32) * weights[
            tap_index
        ].astype(jnp.float32)
    return summed.reshape(values.shape[0], values.shape[1])


def on_device(
    tokens,
    norm_gain,
    proj_u,
    proj_v,
    layer_gain,
    layer_shift,
    mix_weight,
    mix_bias,
    proj_out,
    ffn_gain,
    ffn_gate,
    ffn_value,
    conv_gate,
    conv_value,
    proj_down,
):
    own_width = tokens.shape[1]
    whole_tokens, whole_gain, whole_ffn_gain = (
        lax.all_gather(tokens, "tp", axis=1, tiled=True),
        lax.all_gather(norm_gain, "tp", axis=0, tiled=True),
        lax.all_gather(ffn_gain, "tp", axis=0, tiled=True),
    )
    normed = local_rms(whole_tokens, whole_gain)
    row_count = normed.shape[0]
    whole_u, whole_v = (
        lax.all_gather(proj_u, "fs", axis=0, tiled=True),
        lax.all_gather(proj_v, "fs", axis=0, tiled=True),
    )
    pre_u = matmul(normed, whole_u)
    pre_v = matmul(normed, whole_v)
    act_u = jax.nn.gelu(pre_u, approximate=False)
    act_v = jax.nn.gelu(pre_v, approximate=False)
    full_width = act_v.shape[1] * lax.axis_size("tp")
    total_sum, second = lax.psum((jnp.sum(act_v, axis=1), jnp.sum(act_v * act_v, axis=1)), "tp")
    center = total_sum / full_width
    spread = second / full_width - center * center
    mixed_in = (
        (act_v - center[:, None])
        * lax.rsqrt(spread + EPS)[:, None]
        * layer_gain.astype(jnp.float32)
        + layer_shift.astype(jnp.float32)
    ).astype(jnp.bfloat16)
    groups = mixed_in.shape[1] // GROUP_DIM
    blocks = mixed_in.reshape(row_count // BLOCK, BLOCK, groups, GROUP_DIM)
    segment = jnp.arange(BLOCK) // SEGMENT
    visible = segment[None, :] <= segment[:, None]
    masked = jnp.where(visible[None], mix_weight, jnp.zeros_like(mix_weight))
    spatial = (
        jnp.einsum("gij,njgc->nigc", masked, blocks, preferred_element_type=jnp.float32)
        + mix_bias.astype(jnp.float32).T[None, :, :, None]
    )
    gated_rows = (act_u * spatial.reshape(row_count, mixed_in.shape[1])).astype(jnp.bfloat16)
    whole_out = lax.all_gather(proj_out, "fs", axis=1, tiled=True)
    partial_value = matmul(gated_rows, whole_out)
    summed = lax.psum(partial_value.astype(jnp.bfloat16), "tp").astype(jnp.float32)
    stream_rows = (whole_tokens.astype(jnp.float32) + summed).astype(jnp.bfloat16)
    normed_two = local_rms(stream_rows, whole_ffn_gain)
    stream = lax.dynamic_slice_in_dim(stream_rows, lax.axis_index("tp") * own_width, own_width, 1)
    whole_gate, whole_value = (
        lax.all_gather(ffn_gate, "fs", axis=0, tiled=True),
        lax.all_gather(ffn_value, "fs", axis=0, tiled=True),
    )
    pre_gate = matmul(normed_two, whole_gate)
    pre_value = matmul(normed_two, whole_value)
    conv_g = causal_taps(pre_gate.astype(jnp.bfloat16), conv_gate)
    conv_v = causal_taps(pre_value.astype(jnp.bfloat16), conv_value)
    hidden = (jax.nn.silu(conv_g) * conv_v).astype(jnp.bfloat16)
    whole_down = lax.all_gather(proj_down, "fs", axis=1, tiled=True)
    partial_two = matmul(hidden, whole_down)
    return (
        stream.astype(jnp.float32)
        + lax.psum_scatter(
            partial_two.astype(jnp.bfloat16), "tp", scatter_dimension=1, tiled=True
        ).astype(jnp.float32)
    ).astype(jnp.bfloat16)


def halves(matrix, axis):
    width = matrix.shape[axis] // 2
    return (
        lax.slice_in_dim(matrix, 0, width, axis=axis),
        lax.slice_in_dim(matrix, width, 2 * width, axis=axis),
    )


def own_and_other(matrix, axis, side):
    lower, upper = halves(matrix, axis)
    return jnp.where(side == 0, lower, upper), jnp.where(side == 0, upper, lower)


def in_order(mine, other, side, axis):
    return jnp.concatenate(
        [jnp.where(side == 0, mine, other), jnp.where(side == 0, other, mine)], axis=axis
    )


def after(value, *earlier):
    return lax.optimization_barrier((value,) + earlier)[0]


def on_pair(
    tokens,
    norm_gain,
    proj_u,
    proj_v,
    layer_gain,
    layer_shift,
    mix_weight,
    mix_bias,
    proj_out,
    ffn_gain,
    ffn_gate,
    ffn_value,
    conv_gate,
    conv_value,
    proj_down,
):
    pairs = lax.axis_size("fs") // 2
    depth = pairs // 2
    index = lax.axis_index("fs")
    side, pair = index % 2, index // 2
    core = lax.axis_index("tp")
    spot = jnp.where(pair % 2 == 0, pair // 2, pairs - 1 - pair // 2)
    cycle = [2 * z for z in range(depth)] + [2 * z + 1 for z in reversed(range(depth))]
    right, left = [], []
    for place in range(pairs):
        here, there = cycle[place], cycle[(place + 1) % pairs]
        for one in range(2):
            right.append((2 * here + one, 2 * there + one))
            left.append((2 * there + one, 2 * here + one))
    across = [(2 * one + a, 2 * one + 1 - a) for one in range(pairs) for a in range(2)]

    def swap_side(value):
        return lax.ppermute(value, "fs", across)

    def swap_core(value):
        return lax.ppermute(value, "tp", [(0, 1), (1, 0)])

    def to_ring(values):
        width = values.shape[-1] // pairs
        parts = [values[..., c * width : (c + 1) * width] for c in cycle]
        twice = jnp.concatenate(parts + parts, axis=-1)
        return lax.dynamic_slice_in_dim(twice, spot * width, pairs * width, twice.ndim - 1)

    def from_ring(values):
        width = values.shape[-1] // pairs
        twice = jnp.concatenate([values, values], axis=-1)
        start = ((pairs - spot) % pairs) * width
        ordered = lax.dynamic_slice_in_dim(twice, start, pairs * width, twice.ndim - 1)
        return jnp.concatenate(
            [
                ordered[..., cycle.index(c) * width : (cycle.index(c) + 1) * width]
                for c in range(pairs)
            ],
            axis=-1,
        )

    def ring(chunk, gates):
        pieces = [None] * pairs
        pieces[0] = chunk
        going = [after(chunk, gates[0]), after(chunk, gates[1])] if gates else [chunk, chunk]
        for hop in range(1, depth):
            going = [lax.ppermute(going[0], "fs", right), lax.ppermute(going[1], "fs", left)]
            pieces[pairs - hop], pieces[hop] = going
        first, second = halves(going[0], 0)[0], halves(going[1], 0)[1]
        pieces[depth] = jnp.concatenate(
            [lax.ppermute(first, "fs", right), lax.ppermute(second, "fs", left)], axis=0
        )
        return pieces, going

    def pooled(matrix, split, join, *earlier):
        mine, other = own_and_other(matrix, split, side)
        got = swap_side(after(other, *earlier) if earlier else other)
        return in_order(mine, got, side, join), got

    u_chunk, u_got = pooled(proj_u, 1, 0)
    v_chunk, v_got = pooled(proj_v, 1, 0)
    other_rows = swap_side(after(tokens, u_got, v_got))
    out_chunk, out_got = pooled(proj_out, 0, 1, u_got, v_got)
    gate_chunk, gate_got = pooled(ffn_gate, 1, 0, out_got, other_rows)
    value_chunk, value_got = pooled(ffn_value, 1, 0, out_got, other_rows)
    down_chunk, _ = pooled(proj_down, 0, 1, gate_got, value_got)
    out_chunks, down_chunks = halves(out_chunk, 0), halves(down_chunk, 0)

    u_pieces, gates_a = ring(u_chunk, None)
    v_pieces, gates_b = ring(v_chunk, None)
    out_a, gates_a = ring(out_chunks[0], gates_a)
    out_b, gates_b = ring(out_chunks[1], gates_b)
    gate_pieces, gates_a = ring(gate_chunk, gates_a)
    value_pieces, gates_b = ring(value_chunk, gates_b)
    down_a, _ = ring(down_chunks[0], gates_a)
    down_b, _ = ring(down_chunks[1], gates_b)

    own_half = in_order(tokens, other_rows, side, 0)
    whole_tokens = to_ring(in_order(own_half, swap_core(own_half), core, 1))
    whole_gain = to_ring(lax.all_gather(norm_gain, "tp", axis=0, tiled=True))
    whole_ffn_gain = to_ring(lax.all_gather(ffn_gain, "tp", axis=0, tiled=True))
    normed = local_rms(whole_tokens, whole_gain)
    row_count = normed.shape[0]
    act_v = jax.nn.gelu(matmul(normed, jnp.concatenate(v_pieces, axis=0)), approximate=False)
    sums = jnp.stack([jnp.sum(act_v, axis=1), jnp.sum(act_v * act_v, axis=1)])
    sums = lax.psum(sums, "tp")
    sums = sums + swap_side(sums)
    act_u = jax.nn.gelu(matmul(normed, jnp.concatenate(u_pieces, axis=0)), approximate=False)
    full_width = act_v.shape[1] * lax.axis_size("tp") * 2
    center = sums[0] / full_width
    spread = sums[1] / full_width - center * center
    gain, shift = own_and_other(layer_gain, 0, side)[0], own_and_other(layer_shift, 0, side)[0]
    weight, bias = own_and_other(mix_weight, 0, side)[0], own_and_other(mix_bias, 0, side)[0]
    mixed_in = (
        (act_v - center[:, None]) * lax.rsqrt(spread + EPS)[:, None] * gain.astype(jnp.float32)
        + shift.astype(jnp.float32)
    ).astype(jnp.bfloat16)
    groups = mixed_in.shape[1] // GROUP_DIM
    blocks = mixed_in.reshape(row_count // BLOCK, BLOCK, groups, GROUP_DIM)
    segment = jnp.arange(BLOCK) // SEGMENT
    visible = segment[None, :] <= segment[:, None]
    masked = jnp.where(visible[None], weight, jnp.zeros_like(weight))
    spatial = (
        jnp.einsum("gij,njgc->nigc", masked, blocks, preferred_element_type=jnp.float32)
        + bias.astype(jnp.float32).T[None, :, :, None]
    )
    gated = (act_u * spatial.reshape(row_count, mixed_in.shape[1])).astype(jnp.bfloat16)
    whole_out = jnp.concatenate(
        [jnp.concatenate(out_a, axis=1), jnp.concatenate(out_b, axis=1)], axis=0
    )
    partial_value = matmul(gated, whole_out).astype(jnp.bfloat16)
    mine, other = own_and_other(partial_value, 1, core)
    chip_sum = (mine.astype(jnp.float32) + swap_core(other).astype(jnp.float32)).astype(
        jnp.bfloat16
    )
    summed = chip_sum.astype(jnp.float32) + swap_side(chip_sum).astype(jnp.float32)
    half_tokens = own_and_other(whole_tokens, 1, core)[0]
    half_stream = (half_tokens.astype(jnp.float32) + summed).astype(jnp.bfloat16)
    stream_rows = in_order(half_stream, swap_core(half_stream), core, 1)
    normed_two = local_rms(stream_rows, whole_ffn_gain)
    stream = own_and_other(from_ring(own_and_other(stream_rows, 0, side)[0]), 1, core)[0]

    pre_gate = matmul(normed_two, jnp.concatenate(gate_pieces, axis=0))
    pre_value = matmul(normed_two, jnp.concatenate(value_pieces, axis=0))
    conv_g = causal_taps(pre_gate.astype(jnp.bfloat16), own_and_other(conv_gate, 1, side)[0])
    conv_v = causal_taps(pre_value.astype(jnp.bfloat16), own_and_other(conv_value, 1, side)[0])
    hidden = (jax.nn.silu(conv_g) * conv_v).astype(jnp.bfloat16)
    whole_down = jnp.concatenate(
        [jnp.concatenate(down_a, axis=1), jnp.concatenate(down_b, axis=1)], axis=0
    )
    partial_two = from_ring(matmul(hidden, whole_down).astype(jnp.bfloat16))
    mine, other = own_and_other(partial_two, 1, core)
    chip_sum = (mine.astype(jnp.float32) + swap_core(other).astype(jnp.float32)).astype(
        jnp.bfloat16
    )
    mine, other = own_and_other(chip_sum, 0, side)
    return (
        stream.astype(jnp.float32) + mine.astype(jnp.float32) + swap_side(other).astype(jnp.float32)
    ).astype(jnp.bfloat16)


def solution(mesh):
    paired = mesh.shape["tp"] == 2 and mesh.shape["fs"] % 4 == 0
    in_specs = (
        P("fs", "tp"),
        P("tp"),
        P("fs", "tp"),
        P("fs", "tp"),
        P("tp"),
        P("tp"),
        P("tp", None, None),
        P("tp", None),
        P("tp", "fs"),
        P("tp"),
        P("fs", "tp"),
        P("fs", "tp"),
        P(None, "tp"),
        P(None, "tp"),
        P("tp", "fs"),
    )
    out_specs = P("fs", "tp")
    return jax.shard_map(
        on_pair if paired else on_device, mesh=mesh, in_specs=in_specs, out_specs=out_specs, check_vma=False
    )
```
